32 devices in a mesh: rep: 2 (over x), fs: 8 (over z, y), tp: 2 (over core).
Axes of the slice: x: 2, y: 2, z: 4, core: 2. Of those that a mesh axis runs over, the one named last changes fastest.
Arguments:
- activations: bfloat16 [16384, 1024], P(('rep', 'fs', 'tp')), may hold values from -8 to 8
- mixer_gain: float32 [1024], replicated, may hold values from 0.1 to 1.9
- query_weight: bfloat16 [1024, 256], P('fs', 'tp'), may hold values from -0.1875 to 0.1875
- key_weight: bfloat16 [1024, 256], P('fs', 'tp'), may hold values from -0.1875 to 0.1875
- value_weight: bfloat16 [1024, 512], P('fs', 'tp'), may hold values from -0.1875 to 0.1875
- rank_weight: bfloat16 [1024, 16], replicated, may hold values from -0.1875 to 0.1875
- decay_gate_weight: bfloat16 [16, 256], P(None, 'tp'), may hold values from -1.5 to 1.5
- decay_gate_bias: float32 [256], P('tp'), may hold values from -1.5 to 8
- head_gain: float32 [256], replicated, may hold values from 0.1 to 1.9
- output_weight: bfloat16 [512, 1024], P('tp', 'fs'), may hold values from -0.25 to 0.25
- ffn_gain: float32 [1024], replicated, may hold values from 0.1 to 1.9
- gate_weight: bfloat16 [1024, 2816], P('fs', 'tp'), may hold values from -0.1875 to 0.1875
- up_weight: bfloat16 [1024, 2816], P('fs', 'tp'), may hold values from -0.1875 to 0.1875
- down_weight: bfloat16 [2816, 1024], P('tp', 'fs'), may hold values from -0.109375 to 0.109375
Outputs:
- result: bfloat16 [16384, 1024], P(('rep', 'fs', 'tp'))
The draws below stay inside these ranges and needn't reach their ends.
All inputs are finite; a program needn't handle non-finite values.
Results may differ from the reference program's by a relative error of at most 0.0056.
Values may be sent and summed in bfloat16 or wider, within the bound.
No kernel may reach another device: no remote copies, remote signals or barrier semaphores. Data moves between devices by JAX's collectives and lax.ppermute only.
A program may use at most 64 MiB of HBM per device.

```python
import jax
import jax.numpy as jnp
from jax import lax

D = 1024
FF = 2816
HEADS = 2
DK = 128
DV = 256
RANK = 16
BLOCK = 64
SEQ_LEN = 1024
TOKENS = 16384


def draw_activations(key, part):
    noise_key = jax.random.fold_in(key, 11)
    shift_key = jax.random.fold_in(key, 12)
    shifts = jax.random.normal(shift_key, (TOKENS // BLOCK, 1, D), jnp.float32)
    noise = jax.random.normal(noise_key, (TOKENS // BLOCK, BLOCK, D), jnp.float32)
    combined = noise + 1.5 * shifts
    return jnp.clip(combined, -8.0, 8.0).reshape(TOKENS, D).astype(jnp.bfloat16)


def draw_decay_gate_bias(key, part):
    pick_key = jax.random.fold_in(key, 21)
    low_key = jax.random.fold_in(key, 22)
    high_key = jax.random.fold_in(key, 23)
    channels = HEADS * DK
    forgetful = jax.random.uniform(low_key, (channels,), jnp.float32, -1.5, 0.0)
    hurried = jax.random.uniform(pick_key, (channels,), jnp.float32) < 0.5
    lasting = jax.random.uniform(high_key, (channels,), jnp.float32, 5.0, 8.0)
    return jnp.where(hurried, forgetful, lasting).astype(jnp.float32)


def block_levels(rng, extent, pieces, smallest, top_value):
    loudness = 1.0
    for dim, shards_of in pieces:
        steps = jax.random.uniform(jax.random.fold_in(jax.random.fold_in(rng, 6), dim), (shards_of,), jnp.float32, smallest / len(pieces), top_value / len(pieces))
        loudness = loudness * jnp.repeat(jnp.exp(steps), extent[dim] // shards_of).reshape((-1,) + (1,) * (len(extent) - 1 - dim))
    return loudness


def centred(own_key, extent, width, most, pieces=(), held_as=jnp.bfloat16):
    gain = block_levels(own_key, extent, pieces, -0.22, 0.18) if pieces else 1.0
    entries = jax.random.normal(own_key, extent, jnp.float32) * width * gain
    return jnp.minimum(jnp.maximum(entries, -most), most).astype(held_as)


def setup_inputs(seed: int = 0) -> dict:
    arg_keys = jax.random.split(jax.random.key(seed), 15)
    return {
        "activations": draw_activations(jax.random.fold_in(arg_keys[14], 71), 0),
        "mixer_gain": jnp.clip(1.0 + 0.18 * jax.random.normal(arg_keys[1], (D,), jnp.float32), 0.1, 1.9),
        "query_weight": centred(arg_keys[2], (D, HEADS * DK), D ** -0.5, 0.1875, ((0, 8), (1, 2))),
        "key_weight": centred(arg_keys[3], (D, HEADS * DK), D ** -0.5, 0.1875, ((0, 8), (1, 2))),
        "value_weight": centred(arg_keys[4], (D, HEADS * DV), D ** -0.5, 0.1875, ((0, 8), (1, 2))),
        "rank_weight": centred(arg_keys[5], (D, RANK), D ** -0.5, 0.1875),
        "decay_gate_weight": centred(arg_keys[6], (RANK, HEADS * DK), RANK ** -0.5, 1.5, ((1, 2),)),
        "decay_gate_bias": draw_decay_gate_bias(jax.random.fold_in(arg_keys[14], 71), 0),
        "head_gain": jnp.clip(1.0 + 0.18 * jax.random.normal(arg_keys[8], (DV,), jnp.float32), 0.1, 1.9),
        "output_weight": centred(arg_keys[9], (HEADS * DV, D), (HEADS * DV) ** -0.5, 0.25, ((0, 2), (1, 8))),
        "ffn_gain": jnp.clip(1.0 + 0.18 * jax.random.normal(arg_keys[10], (D,), jnp.float32), 0.1, 1.9),
        "gate_weight": centred(arg_keys[11], (D, FF), D ** -0.5, 0.1875, ((0, 8), (1, 2))),
        "up_weight": centred(arg_keys[12], (D, FF), D ** -0.5, 0.1875, ((0, 8), (1, 2))),
        "down_weight": centred(arg_keys[13], (FF, D), FF ** -0.5, 0.109375, ((0, 2), (1, 8))),
    }


epsilon = 1e-06
decay_softness = 16.0
highest = lax.Precision.HIGHEST

def rms_scale(values, gains):
    values = values.astype(jnp.float32)
    return values * lax.rsqrt(lax.optimization_barrier(jnp.mean(values * values, axis=-1, keepdims=True)) + epsilon) * gains

def linear_attention(queries, keys_all, values_all, decay_logarithm, head_count):
    length = queries.shape[0]
    number = length // BLOCK
    halfway = BLOCK // 2
    causal = jnp.tril(jnp.ones((BLOCK, BLOCK), bool))

    def to_blocks(matrix):
        return matrix.astype(jnp.float32).reshape(number, BLOCK, head_count, matrix.shape[1] // head_count)
    block_query = to_blocks(queries)
    block_key = to_blocks(keys_all)
    block_value = to_blocks(values_all)
    cumulative = jnp.cumsum(to_blocks(decay_logarithm), axis=1)
    middle = cumulative[:, halfway - 1:halfway]
    query_local = block_query * jnp.exp(cumulative - middle)
    key_local = block_key * jnp.exp(middle - cumulative)
    scores = jnp.einsum('nthd,nshd->nhts', query_local, key_local, precision=highest)
    scores = jnp.where(causal[None, None], scores, 0.0)
    within = jnp.einsum('nhts,nshv->nthv', scores, block_value, precision=highest)
    lasting = cumulative[:, -1]
    update = jnp.einsum('nshd,nshv->nhdv', block_key * jnp.exp(lasting[:, None] - cumulative), block_value, precision=highest)

    def advance(memory, inputs):
        fade, addition = inputs
        return (jnp.exp(fade)[:, :, None] * memory + addition, memory)
    key_width = queries.shape[1] // head_count
    value_width = values_all.shape[1] // head_count
    initial = jnp.zeros((head_count, key_width, value_width), jnp.float32)
    earlier = lax.scan(advance, initial, (lasting, update))[1]
    carried = jnp.einsum('nthd,nhdv->nthv', block_query * jnp.exp(cumulative), earlier, precision=highest)
    return (within + carried).reshape(length, head_count, value_width)

def reference(activations, mixer_gain, query_weight, key_weight, value_weight, rank_weight, decay_gate_weight, decay_gate_bias, head_gain, output_weight, ffn_gain, gate_weight, up_weight, down_weight):

    def one_sequence(tokens):
        residual = tokens.astype(jnp.float32)
        normed = rms_scale(residual, mixer_gain).astype(jnp.bfloat16)
        rank_slice = jnp.dot(normed, rank_weight, preferred_element_type=jnp.float32).astype(jnp.bfloat16)
        queries = jnp.dot(normed, query_weight, preferred_element_type=jnp.float32).astype(jnp.bfloat16)
        keys_all = jnp.dot(normed, key_weight, preferred_element_type=jnp.float32).astype(jnp.bfloat16)
        values_all = jnp.dot(normed, value_weight, preferred_element_type=jnp.float32).astype(jnp.bfloat16)
        decay_logarithm = jax.nn.log_sigmoid(jnp.dot(rank_slice, decay_gate_weight, preferred_element_type=jnp.float32) + decay_gate_bias) / decay_softness
        attended = linear_attention(queries, keys_all, values_all, decay_logarithm, HEADS)
        head_rows = rms_scale(attended, head_gain).astype(jnp.bfloat16).reshape(SEQ_LEN, HEADS * DV)
        mixed = residual + jnp.dot(head_rows, output_weight, preferred_element_type=jnp.float32)
        ffn_normed = rms_scale(mixed, ffn_gain).astype(jnp.bfloat16)
        gate_sum = jnp.dot(ffn_normed, gate_weight, preferred_element_type=jnp.float32)
        up_sum = jnp.dot(ffn_normed, up_weight, preferred_element_type=jnp.float32)
        hidden = (jax.nn.silu(gate_sum) * up_sum).astype(jnp.bfloat16)
        return (mixed + jnp.dot(hidden, down_weight, preferred_element_type=jnp.float32)).astype(jnp.bfloat16)
    outputs = lax.map(one_sequence, activations.reshape(TOKENS // SEQ_LEN, SEQ_LEN, D))
    return outputs.reshape(TOKENS, D)
```

```python
import functools

import jax
import jax.numpy as jnp
from jax import lax
from jax.experimental import pallas as pl
from jax.experimental.pallas import tpu as pltpu
from jax.sharding import PartitionSpec as P

DK = 128
DV = 256
BLOCK = 64

epsilon = 1e-06
decay_softness = 16.0


def rms_scale(values, gains):
    return values * lax.rsqrt(jnp.mean(values * values, axis=-1, keepdims=True) + epsilon) * gains


def dot_nt(a, b):
    return lax.dot_general(a, b, (((1,), (1,)), ((), ())), preferred_element_type=jnp.float32)


def dot_tn(a, b):
    return lax.dot_general(a, b, (((0,), (0,)), ((), ())), preferred_element_type=jnp.float32)


def mixer_kernel(
    side, own, other, gain, wqkv, wrank, wdecay, bias, head_gain, out, normed, qkv, logs, *, heads
):
    rows = own.shape[0]
    length = 2 * rows
    step = min(128, rows)
    here = side[0]
    for i in range(rows // step):
        for source, place in ((own, here), (other, 1 - here)):
            x = source[pl.ds(i * step, step), :].astype(jnp.float32)
            start = pl.multiple_of(place * rows + i * step, step)
            normed[pl.ds(start, step), :] = rms_scale(x, gain[...]).astype(jnp.bfloat16)
    for i in range(length // 256):
        part = normed[pl.ds(i * 256, 256), :]
        qkv[pl.ds(i * 256, 256), :] = jnp.dot(
            part, wqkv[...], preferred_element_type=jnp.float32
        ).astype(jnp.bfloat16)
        ranked = jnp.dot(part, wrank[...], preferred_element_type=jnp.float32).astype(jnp.bfloat16)
        z = jnp.dot(ranked, wdecay[...], preferred_element_type=jnp.float32) + bias[...]
        logs[pl.ds(i * 256, 256), :] = (
            jnp.minimum(z, 0.0) - jnp.log1p(jnp.exp(-jnp.abs(z)))
        ) / decay_softness
    row = lax.broadcasted_iota(jnp.int32, (BLOCK, BLOCK), 0)
    col = lax.broadcasted_iota(jnp.int32, (BLOCK, BLOCK), 1)
    causal = row >= col
    ones = jnp.where(causal, 1.0, 0.0).astype(jnp.float32)
    half = BLOCK // 2
    for h in range(heads):
        state = jnp.zeros((DV, DK), jnp.float32)
        for n in range(length // BLOCK):
            at = pl.ds(n * BLOCK, BLOCK)
            q = qkv[at, h * DK : (h + 1) * DK].astype(jnp.float32)
            k = qkv[at, (heads + h) * DK : (heads + h + 1) * DK].astype(jnp.float32)
            v = qkv[at, 2 * heads * DK + h * DV : 2 * heads * DK + (h + 1) * DV]
            g = logs[at, h * DK : (h + 1) * DK]
            cum = jnp.dot(
                ones, g, precision=lax.Precision.HIGHEST, preferred_element_type=jnp.float32
            )
            mid = cum[half - 1 : half]
            last = cum[BLOCK - 1 : BLOCK]
            q_local = (q * jnp.exp(cum - mid)).astype(jnp.bfloat16)
            k_local = (k * jnp.exp(mid - cum)).astype(jnp.bfloat16)
            scores = jnp.where(causal, dot_nt(q_local, k_local), 0.0).astype(jnp.bfloat16)
            attended = jnp.dot(scores, v, preferred_element_type=jnp.float32)
            if n > 0:
                q_far = (q * jnp.exp(cum)).astype(jnp.bfloat16)
                attended = attended + dot_nt(q_far, state.astype(jnp.bfloat16))
            k_far = (k * jnp.exp(last - cum)).astype(jnp.bfloat16)
            state = jnp.exp(last) * state + dot_tn(v, k_far)
            out[at, h * DV : (h + 1) * DV] = rms_scale(attended, head_gain[...]).astype(
                jnp.bfloat16
            )


def ring_pieces(shard, axis, order):
    n = len(order)
    ahead = [(order[i], order[(i + 1) % n]) for i in range(n)]
    behind = [(b, a) for a, b in ahead]
    pieces = {0: shard}
    up = down = shard
    for k in range(1, (n - 1) // 2 + 1):
        up = lax.ppermute(up, axis, ahead)
        down = lax.ppermute(down, axis, behind)
        pieces[-k] = up
        pieces[k] = down
    if n % 2 == 0:
        cut = shard.shape[0] // 2
        pieces[n // 2] = jnp.concatenate(
            [lax.ppermute(up[:cut], axis, ahead), lax.ppermute(down[cut:], axis, behind)], axis=0
        )
    return pieces


def assemble(pieces, place, order):
    n = len(order)
    table = jnp.asarray(order, jnp.int32)
    rows, width = pieces[0].shape
    full = jnp.zeros((n, rows, width), pieces[0].dtype)
    for k, piece in pieces.items():
        block = table[(place + k + n) % n]
        full = lax.dynamic_update_slice(full, piece[None], (block, 0, 0))
    return full.reshape(n * rows, width)


def after(value, *earlier):
    return lax.optimization_barrier((value, *earlier))[0]


def local(
    sizes,
    activations,
    mixer_gain,
    query_weight,
    key_weight,
    value_weight,
    rank_weight,
    decay_gate_weight,
    decay_gate_bias,
    head_gain,
    output_weight,
    ffn_gain,
    gate_weight,
    up_weight,
    down_weight,
):
    n = sizes["fs"]
    order = list(range(0, n, 2)) + list(range(1, n, 2))[::-1]
    inverse = [order.index(i) for i in range(n)]
    place = jnp.asarray(inverse, jnp.int32)[lax.axis_index("fs")]
    side = lax.axis_index("tp").astype(jnp.int32)
    swap = [(0, 1), (1, 0)]
    rows, width = activations.shape
    heads = query_weight.shape[1] // DK
    hidden_width = gate_weight.shape[1]

    def peer(x):
        return lax.ppermute(x, "tp", swap)

    qkv_shard = jnp.concatenate([query_weight, key_weight, value_weight], axis=1)
    qkv_pieces = ring_pieces(qkv_shard, "fs", order)
    other = peer(activations)
    out_shard = after(output_weight.T, qkv_pieces[1], qkv_pieces[-1])
    out_pieces = ring_pieces(out_shard, "fs", order)
    held = (qkv_pieces[2 % n], qkv_pieces[-2 % n if n < 4 else -2])
    gate_pieces = ring_pieces(after(gate_weight, *held), "fs", order)
    up_pieces = ring_pieces(after(up_weight, *held), "fs", order)
    down_pieces = ring_pieces(after(down_weight.T, *held), "fs", order)

    qkv_full = assemble(qkv_pieces, place, order)
    vmem = pl.BlockSpec(memory_space=pltpu.VMEM)
    head_rows = pl.pallas_call(
        functools.partial(mixer_kernel, heads=heads),
        out_shape=jax.ShapeDtypeStruct((2 * rows, heads * DV), jnp.bfloat16),
        in_specs=[pl.BlockSpec(memory_space=pltpu.SMEM)] + [vmem] * 8,
        out_specs=vmem,
        scratch_shapes=[
            pltpu.VMEM((2 * rows, width), jnp.bfloat16),
            pltpu.VMEM((2 * rows, heads * (2 * DK + DV)), jnp.bfloat16),
            pltpu.VMEM((2 * rows, heads * DK), jnp.float32),
        ],
        name="mixer",
    )(
        side[None],
        activations,
        other,
        mixer_gain[None],
        qkv_full,
        rank_weight,
        decay_gate_weight,
        decay_gate_bias[None],
        head_gain[None],
    )
    out_full = assemble(out_pieces, place, order)
    out_peer = peer(out_full)
    mine = lax.dynamic_slice(head_rows, (side * rows, 0), (rows, head_rows.shape[1]))
    theirs = lax.dynamic_slice(head_rows, ((1 - side) * rows, 0), (rows, head_rows.shape[1]))
    recv = peer(theirs)
    mixed = activations.astype(jnp.float32) + dot_nt(mine, out_full) + dot_nt(recv, out_peer)
    ffn_own = rms_scale(mixed, ffn_gain).astype(jnp.bfloat16)
    ffn_other = peer(ffn_own)
    gate_full = assemble(gate_pieces, place, order)
    up_full = assemble(up_pieces, place, order)
    down_full = assemble(down_pieces, place, order)

    def hidden_of(x):
        gate = jnp.dot(x, gate_full, preferred_element_type=jnp.float32)
        up = jnp.dot(x, up_full, preferred_element_type=jnp.float32)
        return (jax.nn.silu(gate) * up).astype(jnp.bfloat16)

    hidden_other = hidden_of(ffn_other)
    hidden_own = hidden_of(ffn_own)
    away = peer(dot_nt(hidden_other, down_full).astype(jnp.bfloat16))
    result = mixed + dot_nt(hidden_own, down_full) + away.astype(jnp.float32)
    return result.astype(jnp.bfloat16)


def solution(mesh):
    in_specs = (
        P(("rep", "fs", "tp"), None),
        P(),
        P("fs", "tp"),
        P("fs", "tp"),
        P("fs", "tp"),
        P(),
        P(None, "tp"),
        P("tp"),
        P(),
        P("tp", "fs"),
        P(),
        P("fs", "tp"),
        P("fs", "tp"),
        P("tp", "fs"),
    )
    out_specs = P(("rep", "fs", "tp"), None)
    return jax.shard_map(
        functools.partial(local, dict(mesh.shape)),
        mesh=mesh,
        in_specs=in_specs,
        out_specs=out_specs,
        check_vma=False,
    )
```

```python
import functools

import jax
import jax.numpy as jnp
from jax import lax
from jax.experimental import pallas as pl
from jax.experimental.pallas import tpu as pltpu
from jax.sharding import PartitionSpec as P

DK = 128
DV = 256
BLOCK = 64

epsilon = 1e-06
decay_softness = 16.0


def rms_scale(values, gains):
    return values * lax.rsqrt(jnp.mean(values * values, axis=-1, keepdims=True) + epsilon) * gains


def dot_nt(a, b):
    return lax.dot_general(a, b, (((1,), (1,)), ((), ())), preferred_element_type=jnp.float32)


def dot_tn(a, b):
    return lax.dot_general(a, b, (((0,), (0,)), ((), ())), preferred_element_type=jnp.float32)


def block_at(position, n):
    evens = (n + 1) // 2
    position = lax.rem(position + 2 * n, n)
    return jnp.where(position < evens, 2 * position, 2 * (n - position) - 1)


def ring_place(n):
    index = lax.axis_index("fs")
    half = lax.div(index, 2)
    return jnp.where(lax.rem(index, 2) == 0, half, n - 1 - half)


def spread(refs, spots, target, n, lead=None):
    place = ring_place(n)
    for (k, offset), ref in zip(spots, refs):
        rows = ref.shape[0]
        size = target.shape[-2] // n
        start = block_at(place + k, n) * size + offset
        start = pl.multiple_of(start, 16)
        if lead is None:
            target[pl.ds(start, rows), :] = ref[...]
        else:
            target[lead, pl.ds(start, rows), :] = ref[...]


def pack_kernel(q, k, v, o, out):
    at = 0
    for ref in (q, k, v, o):
        out[:, at : at + ref.shape[1]] = ref[...]
        at += ref.shape[1]


def pick_kernel(gate, up, out):
    rep = lax.axis_index("rep")

    @pl.when(lax.rem(rep, 2) == 0)
    def _():
        out[...] = gate[...]

    @pl.when(lax.rem(rep, 2) == 1)
    def _():
        out[...] = up[...]


def mixer_kernel(own, other, gain, wrank, wdecay, bias, head_gain, *refs, heads, spots, n):
    pieces = refs[: len(spots)]
    part, part16, weights, normed, qkv, logs, head_rows = refs[len(spots) :]
    rows = own.shape[0]
    length = 2 * rows
    step = min(128, rows)
    here = lax.axis_index("tp")
    spread(pieces, spots, weights, n)
    for i in range(rows // step):
        for source, place in ((own, here), (other, 1 - here)):
            x = source[pl.ds(i * step, step), :].astype(jnp.float32)
            start = pl.multiple_of(place * rows + i * step, step)
            normed[pl.ds(start, step), :] = rms_scale(x, gain[...]).astype(jnp.bfloat16)
    narrow = qkv.shape[1]

    @pl.loop(0, length // 256)
    def _(i):
        at = pl.ds(pl.multiple_of(i * 256, 256), 256)
        piece = normed[at, :]
        qkv[at, :] = jnp.dot(
            piece, weights[:, :narrow], preferred_element_type=jnp.float32
        ).astype(jnp.bfloat16)
        ranked = dot_nt(piece, wrank[...]).astype(jnp.bfloat16)
        z = jnp.dot(ranked, wdecay[...], preferred_element_type=jnp.float32) + bias[...]
        logs[at, :] = (
            jnp.minimum(z, 0.0) - jnp.log1p(jnp.exp(-jnp.abs(z)))
        ) / decay_softness
    row = lax.broadcasted_iota(jnp.int32, (BLOCK, BLOCK), 0)
    col = lax.broadcasted_iota(jnp.int32, (BLOCK, BLOCK), 1)
    causal = row >= col
    ones = jnp.where(causal, 1.0, 0.0).astype(jnp.float32)
    half = BLOCK // 2
    for h in range(heads):
        state = jnp.zeros((DV, DK), jnp.float32)
        for n in range(length // BLOCK):
            at = pl.ds(n * BLOCK, BLOCK)
            q = qkv[at, h * DK : (h + 1) * DK].astype(jnp.float32)
            k = qkv[at, (heads + h) * DK : (heads + h + 1) * DK].astype(jnp.float32)
            v = qkv[at, 2 * heads * DK + h * DV : 2 * heads * DK + (h + 1) * DV]
            g = logs[at, h * DK : (h + 1) * DK]
            cum = jnp.dot(
                ones, g, precision=lax.Precision.HIGHEST, preferred_element_type=jnp.float32
            )
            mid = cum[half - 1 : half]
            last = cum[BLOCK - 1 : BLOCK]
            q_local = (q * jnp.exp(cum - mid)).astype(jnp.bfloat16)
            k_local = (k * jnp.exp(mid - cum)).astype(jnp.bfloat16)
            scores = jnp.where(causal, dot_nt(q_local, k_local), 0.0).astype(jnp.bfloat16)
            attended = jnp.dot(scores, v, preferred_element_type=jnp.float32)
            if n > 0:
                q_far = (q * jnp.exp(cum)).astype(jnp.bfloat16)
                attended = attended + dot_nt(q_far, state.astype(jnp.bfloat16))
            k_far = (k * jnp.exp(last - cum)).astype(jnp.bfloat16)
            state = jnp.exp(last) * state + dot_tn(v, k_far)
            head_rows[at, h * DV : (h + 1) * DV] = rms_scale(attended, head_gain[...]).astype(
                jnp.bfloat16
            )

    @pl.loop(0, length // 256)
    def _(i):
        at = pl.ds(pl.multiple_of(i * 256, 256), 256)
        share = dot_nt(head_rows[at, :], weights[:, narrow:])
        part[at, :] = share
        part16[at, :] = share.astype(jnp.bfloat16)


def hidden_kernel(own, other, part, recv, gain, gate, up, *refs, spots, n):
    m = len(spots)
    mine = refs[:m]
    theirs = refs[m : 2 * m]
    hidden, mixed, weights, normed = refs[2 * m :]
    rows = own.shape[0]
    step = min(128, rows)
    here = lax.axis_index("tp")
    rep = lax.rem(lax.axis_index("rep"), 2)
    spread([gate], [(0, 0)], weights, n, 0)
    spread([up], [(0, 0)], weights, n, 1)
    spread(mine, spots, weights, n, rep)
    spread(theirs, spots, weights, n, 1 - rep)
    for i in range(rows // step):
        for source, place in ((own, here), (other, 1 - here)):
            local_at = pl.ds(i * step, step)
            at = pl.ds(pl.multiple_of(place * rows + i * step, step), step)
            x = source[local_at, :].astype(jnp.float32) + part[at, :]
            x = x + recv[at, :].astype(jnp.float32)
            if source is own:
                mixed[local_at, :] = x
            normed[at, :] = rms_scale(x, gain[...]).astype(jnp.bfloat16)

    @pl.loop(0, 2 * rows // 128)
    def _(i):
        at = pl.ds(pl.multiple_of(i * 128, 128), 128)
        x = normed[at, :]
        g = jnp.dot(x, weights[0], preferred_element_type=jnp.float32)
        u = jnp.dot(x, weights[1], preferred_element_type=jnp.float32)
        hidden[at, :] = (g / (1.0 + jnp.exp(-g)) * u).astype(jnp.bfloat16)


def away_kernel(hidden, *refs, spots, n):
    pieces = refs[: len(spots)]
    away, full = refs[len(spots) :]
    rows = away.shape[0]
    spread(pieces, spots, full, n)
    there = 1 - lax.axis_index("tp")
    step = min(256, rows)
    for i in range(rows // step):
        at = pl.ds(pl.multiple_of(there * rows + i * step, step), step)
        away[pl.ds(i * step, step), :] = dot_nt(hidden[at, :], full[...]).astype(jnp.bfloat16)


def stay_kernel(hidden, mixed, full, stay):
    rows = stay.shape[0]
    here = lax.axis_index("tp")
    step = min(256, rows)
    for i in range(rows // step):
        at = pl.ds(pl.multiple_of(here * rows + i * step, step), step)
        near = pl.ds(i * step, step)
        stay[near, :] = mixed[near, :] + dot_nt(hidden[at, :], full[...])


def ring_pieces(shard, axis, order):
    n = len(order)
    ahead = [(order[i], order[(i + 1) % n]) for i in range(n)]
    behind = [(b, a) for a, b in ahead]
    pieces = {(0, 0): shard}
    up = down = shard
    for k in range(1, (n - 1) // 2 + 1):
        up = lax.ppermute(up, axis, ahead)
        down = lax.ppermute(down, axis, behind)
        pieces[-k, 0] = up
        pieces[k, 0] = down
    if n % 2 == 0:
        cut = shard.shape[0] // 2
        pieces[n // 2, 0] = lax.ppermute(up[:cut], axis, ahead)
        pieces[n // 2, cut] = lax.ppermute(down[cut:], axis, behind)
    return pieces


def after(value, *earlier):
    return lax.optimization_barrier((value, *earlier))[0]


vmem = pl.BlockSpec(memory_space=pltpu.VMEM)


def kernel(body, outs, scratch, name):
    def call(*args):
        return pl.pallas_call(
            body,
            out_shape=outs,
            in_specs=[vmem] * len(args),
            out_specs=jax.tree.map(lambda _: vmem, outs),
            scratch_shapes=scratch,
            name=name,
        )(*args)

    return call


def local(
    sizes,
    activations,
    mixer_gain,
    query_weight,
    key_weight,
    value_weight,
    rank_weight,
    decay_gate_weight,
    decay_gate_bias,
    head_gain,
    output_weight,
    ffn_gain,
    gate_weight,
    up_weight,
    down_weight,
):
    n = sizes["fs"]
    order = list(range(0, n, 2)) + list(range(1, n, 2))[::-1]
    swap = [(0, 1), (1, 0)]
    rep_swap = [(i, i ^ 1) for i in range(sizes["rep"])]
    rows, width = activations.shape
    heads = query_weight.shape[1] // DK
    units = gate_weight.shape[1]
    shard_rows = gate_weight.shape[0]
    bf16, f32 = jnp.bfloat16, jnp.float32
    shape = jax.ShapeDtypeStruct

    def peer(x):
        return lax.ppermute(x, "tp", swap)

    narrow = heads * (2 * DK + DV)
    wide = narrow + heads * DV
    pack = kernel(pack_kernel, shape((shard_rows, wide), bf16), [], "pack")
    first = pack(query_weight, key_weight, value_weight, output_weight.T)
    other = peer(activations)
    first_pieces = ring_pieces(first, "fs", order)
    picked = kernel(pick_kernel, shape(gate_weight.shape, bf16), [], "pick")(gate_weight, up_weight)
    last = (n - 1) // 2
    picked = after(picked, first_pieces[1, 0], first_pieces[-1, 0])
    down_shard = after(down_weight.T, first_pieces[last, 0], first_pieces[-last, 0])
    mine = ring_pieces(picked, "fs", order)
    mine.pop((0, 0))
    theirs = {k: lax.ppermute(x, "rep", rep_swap) for k, x in mine.items()}
    down_pieces = ring_pieces(down_shard, "fs", order)

    spots = tuple(first_pieces)
    length = 2 * rows
    part, part16 = kernel(
        functools.partial(mixer_kernel, heads=heads, spots=spots, n=n),
        (shape((length, width), f32), shape((length, width), bf16)),
        [
            pltpu.VMEM((width, wide), bf16),
            pltpu.VMEM((length, width), bf16),
            pltpu.VMEM((length, narrow), bf16),
            pltpu.VMEM((length, heads * DK), f32),
            pltpu.VMEM((length, heads * DV), bf16),
        ],
        "mixer",
    )(
        activations,
        other,
        mixer_gain[None],
        rank_weight.T,
        decay_gate_weight,
        decay_gate_bias[None],
        head_gain[None],
        *first_pieces.values(),
    )
    recv = peer(part16)
    hidden, mixed = kernel(
        functools.partial(hidden_kernel, spots=tuple(mine), n=n),
        (shape((length, units), bf16), shape((rows, width), f32)),
        [pltpu.VMEM((2, width, units), bf16), pltpu.VMEM((length, width), bf16)],
        "hidden",
    )(
        activations,
        other,
        part,
        recv,
        ffn_gain[None],
        gate_weight,
        up_weight,
        *mine.values(),
        *theirs.values(),
    )
    away, full = kernel(
        functools.partial(away_kernel, spots=tuple(down_pieces), n=n),
        (shape((rows, width), bf16), shape((width, units), bf16)),
        [],
        "away",
    )(hidden, *down_pieces.values())
    back = peer(away)
    stay = kernel(stay_kernel, shape((rows, width), f32), [], "stay")(hidden, mixed, full)
    return (stay + back.astype(f32)).astype(bf16)


def solution(mesh):
    in_specs = (
        P(("rep", "fs", "tp"), None),
        P(),
        P("fs", "tp"),
        P("fs", "tp"),
        P("fs", "tp"),
        P(),
        P(None, "tp"),
        P("tp"),
        P(),
        P("tp", "fs"),
        P(),
        P("fs", "tp"),
        P("fs", "tp"),
        P("tp", "fs"),
    )
    out_specs = P(("rep", "fs", "tp"), None)
    return jax.shard_map(
        functools.partial(local, dict(mesh.shape)),
        mesh=mesh,
        in_specs=in_specs,
        out_specs=out_specs,
        check_vma=False,
    )
```
